512 devices in a mesh: sp: 64 (over z, y), tp: 8 (over x, core).
Axes of the slice: x: 4, y: 4, z: 16, core: 2. Of those that a mesh axis runs over, the one named last changes fastest.
Arguments:
- tokens: bfloat16 [16384, 2048], P('sp', 'tp'), may hold values from -6 to 6
- norm_gain: float32 [2048], replicated, may hold values from 0.1 to 1.9
- query_weight: bfloat16 [2048, 1024], P(None, 'tp'), may hold values from -0.18782524 to 0.18782524
- key_weight: bfloat16 [2048, 1024], P(None, 'tp'), may hold values from -0.18782524 to 0.18782524
- value_weight: bfloat16 [2048, 1024], P(None, 'tp'), may hold values from -0.125 to 0.125
- gate_weight: bfloat16 [2048, 1024], P(None, 'tp'), may hold values from -0.125 to 0.125
- outer_weight: bfloat16 [2048, 1024], P(None, 'tp'), may hold values from -0.125 to 0.125
- inner_weight: bfloat16 [2048, 1024], P(None, 'tp'), may hold values from -0.125 to 0.125
- signal_weight: bfloat16 [2048, 1024], P(None, 'tp'), may hold values from -0.125 to 0.125
- conv_taps: float32 [3, 1024], P(None, 'tp'), may hold values from -3.5 to 3.5
- lambdas: float32 [8], P('tp'), may hold values from 0.3 to 0.8
- head_gain: float32 [1024], P('tp'), may hold values from 0.1 to 1.9
- attn_out_weight: bfloat16 [1024, 2048], P('tp'), may hold values from -0.125 to 0.125
- conv_out_weight: bfloat16 [1024, 2048], P('tp'), may hold values from -0.125 to 0.125
Outputs:
- mixed: bfloat16 [16384, 2048], P(('sp', 'tp'))
- log_totals: float32 [8, 2, 16384], P('tp', None, 'sp')
The draws below stay inside these ranges and needn't reach their ends.
All inputs are finite; a program needn't handle non-finite values.
Results may differ from the reference program's by a relative error of at most 0.014.
Values may be sent and summed in bfloat16 or wider, within the bound.
No kernel may reach another device: no remote copies, remote signals or barrier semaphores. Data moves between devices by JAX's collectives and lax.ppermute only.
A program may use at most 64 MiB of HBM per device.

```python
import jax
import jax.numpy as jnp
from jax import lax

D = 2048
HEADS = 8
QK = 64
VD = 128
CONV = 1024
KERNEL = 3
TOKENS = 16384
N_TP = 8


def projection_pair(key):
    columns = HEADS * 2 * QK
    spread = 1.4 * D ** (-0.5)
    query_part = jnp.clip(jax.random.normal(jax.random.fold_in(key, 101), (D, columns), jnp.float32), -6.0, 6.0) * spread
    key_part = jnp.clip(jax.random.normal(jax.random.fold_in(key, 102), (D, columns), jnp.float32), -6.0, 6.0) * spread
    return (query_part, key_part)


def draw_query_weight(key, part):
    return projection_pair(key)[0].astype(jnp.bfloat16)


def draw_key_weight(key, part):
    return projection_pair(key)[1].astype(jnp.bfloat16)


def draw_tokens(key, part):
    base = jnp.clip(jax.random.normal(jax.random.fold_in(key, 201), (TOKENS, D), jnp.float32), -6.0, 6.0)
    return base.astype(jnp.bfloat16)


def steps_of(own_key, extent, cuts, smallest, high):
    def one(axis_at, parts):
        heights = jax.random.uniform(jax.random.fold_in(jax.random.fold_in(own_key, 6), axis_at), (parts,), jnp.float32, smallest / len(cuts), high / len(cuts))
        return jnp.repeat(jnp.exp(heights), extent[axis_at] // parts).reshape((-1,) + (1,) * (len(extent) - axis_at - 1))

    loudness = one(*cuts[0])
    for cut in cuts[1:]:
        loudness = loudness * one(*cut)
    return loudness


def noise(key, shape, scale, reach, split=(), kind=jnp.bfloat16):
    factor_of = steps_of(key, shape, split, -0.22, 0.18) if split else 1.0
    array = jax.random.normal(key, shape, jnp.float32) * scale * factor_of
    return jnp.minimum(jnp.maximum(array, -reach), reach).astype(kind)


def setup_inputs(seed: int = 0) -> dict:
    arg_keys = jax.random.split(jax.random.key(seed), 15)
    tokens = draw_tokens(jax.random.fold_in(arg_keys[14], 71), 0)
    norm_gain = jnp.clip(1.0 + 0.18 * jax.random.normal(arg_keys[1], (D,), jnp.float32), 0.1, 1.9)
    query_weight = draw_query_weight(jax.random.fold_in(arg_keys[14], 71), 0)
    key_weight = draw_key_weight(jax.random.fold_in(arg_keys[14], 71), 0)
    value_weight = noise(arg_keys[4], (D, HEADS * VD), D ** -0.5, 0.125, ((1, 8),))
    gate_weight = noise(arg_keys[5], (D, HEADS * VD), D ** -0.5, 0.125, ((1, 8),))
    outer_weight = noise(arg_keys[6], (D, CONV), D ** -0.5, 0.125, ((1, 8),))
    inner_weight = noise(arg_keys[7], (D, CONV), D ** -0.5, 0.125, ((1, 8),))
    signal_weight = noise(arg_keys[8], (D, CONV), D ** -0.5, 0.125, ((1, 8),))
    conv_taps = noise(arg_keys[9], (KERNEL, CONV), KERNEL ** -0.5, 3.5, ((1, 8),), jnp.float32)
    lambdas = jnp.clip(0.3 + 0.5 * jax.random.uniform(arg_keys[10], (HEADS,), jnp.float32) ** steps_of(arg_keys[10], (HEADS,), ((0, 8),), -0.2, 0.2), 0.3, 0.8)
    head_gain = jnp.clip(1.0 + 0.18 * jax.random.normal(arg_keys[11], (HEADS * VD,), jnp.float32), 0.1, 1.9)
    attn_out_weight = noise(arg_keys[12], (HEADS * VD, D), (HEADS * VD + CONV) ** -0.5, 0.125, ((0, 8),))
    conv_out_weight = noise(arg_keys[13], (CONV, D), (HEADS * VD + CONV) ** -0.5, 0.125, ((0, 8),))
    return dict(tokens=tokens, norm_gain=norm_gain, query_weight=query_weight, key_weight=key_weight, value_weight=value_weight, gate_weight=gate_weight, outer_weight=outer_weight, inner_weight=inner_weight, signal_weight=signal_weight, conv_taps=conv_taps, lambdas=lambdas, head_gain=head_gain, attn_out_weight=attn_out_weight, conv_out_weight=conv_out_weight)


def reference(tokens, norm_gain, query_weight, key_weight, value_weight, gate_weight, outer_weight, inner_weight, signal_weight, conv_taps, lambdas, head_gain, attn_out_weight, conv_out_weight):
    tokens_f = tokens.astype(jnp.float32)
    scale = lax.rsqrt(lax.optimization_barrier(jnp.mean(tokens_f * tokens_f, axis=-1, keepdims=True)) + 1e-06)
    normed_in = (tokens_f * norm_gain).astype(jnp.bfloat16)

    def project(weight):
        return (jnp.dot(normed_in.astype(jnp.float32), weight.astype(jnp.float32), preferred_element_type=jnp.float32) * scale).astype(jnp.bfloat16)
    query = project(query_weight)
    key = project(key_weight)
    value = project(value_weight)
    attn_gate = project(gate_weight)
    outer = project(outer_weight)
    inner = project(inner_weight)
    signal = project(signal_weight)
    query_heads = query.reshape(TOKENS, HEADS, 2, QK)
    key_heads = key.reshape(TOKENS, HEADS, 2, QK).astype(jnp.float32)
    value_heads = value.reshape(TOKENS, HEADS, VD).astype(jnp.float32)
    block_rows = 256 if TOKENS % 256 == 0 else 128
    key_pos = jnp.arange(TOKENS, dtype=jnp.int32)

    def one_block(index):
        query_block = lax.dynamic_slice_in_dim(query_heads, (index * block_rows).astype(jnp.int32), block_rows, 0).astype(jnp.float32)
        query_pos = index * block_rows + jnp.arange(block_rows, dtype=jnp.int32)
        score = jnp.einsum('qhmd,khmd->hmqk', query_block, key_heads) * QK ** (-0.5)
        visible = query_pos[:, None] >= key_pos[None, :]
        score = jnp.where(visible, score, -1e+30)
        top = lax.optimization_barrier(jnp.max(score, axis=-1, keepdims=True))
        weights = jnp.exp(score - top)
        total = lax.optimization_barrier(jnp.sum(weights, axis=-1, keepdims=True))
        summed = jnp.einsum('hmqk,khd->hmqd', weights.astype(jnp.bfloat16).astype(jnp.float32), value_heads)
        mapped = summed / total
        diff = mapped[:, 0] - lambdas[:, None, None] * mapped[:, 1]
        log_total = jnp.log(total[..., 0]) + top[..., 0]
        return (jnp.transpose(diff, (1, 0, 2)), log_total)
    diffs, log_parts = lax.map(one_block, jnp.arange(TOKENS // block_rows, dtype=jnp.int32))
    diff = diffs.reshape(TOKENS, HEADS, VD)
    log_totals = jnp.transpose(log_parts, (1, 2, 0, 3)).reshape(HEADS, 2, TOKENS)
    normed = diff * lax.rsqrt(lax.optimization_barrier(jnp.mean(diff * diff, axis=-1, keepdims=True)) + 1e-05) * head_gain.reshape(HEADS, VD)
    head_out = (normed.reshape(TOKENS, HEADS * VD) * jax.nn.silu(attn_gate.astype(jnp.float32))).astype(jnp.bfloat16)
    inner_sig = (inner.astype(jnp.float32) * signal.astype(jnp.float32)).astype(jnp.bfloat16)
    padded = jnp.pad(inner_sig.astype(jnp.float32), ((KERNEL - 1, 0), (0, 0)))
    convolved = jnp.zeros((TOKENS, CONV), jnp.float32)
    for offset in range(KERNEL):
        convolved = convolved + conv_taps[offset] * padded[offset:offset + TOKENS]
    conv_out = (outer.astype(jnp.float32) * convolved).astype(jnp.bfloat16)
    head_cols = HEADS * VD // N_TP
    conv_cols = CONV // N_TP

    def add_group(accum, group):
        head_part = lax.dynamic_slice_in_dim(head_out, (group * head_cols).astype(jnp.int32), head_cols, 1)
        head_rows = lax.dynamic_slice_in_dim(attn_out_weight, (group * head_cols).astype(jnp.int32), head_cols, 0)
        conv_part = lax.dynamic_slice_in_dim(conv_out, (group * conv_cols).astype(jnp.int32), conv_cols, 1)
        conv_rows = lax.dynamic_slice_in_dim(conv_out_weight, (group * conv_cols).astype(jnp.int32), conv_cols, 0)
        partial_value = jnp.dot(head_part.astype(jnp.float32), head_rows.astype(jnp.float32), preferred_element_type=jnp.float32) + jnp.dot(conv_part.astype(jnp.float32), conv_rows.astype(jnp.float32), preferred_element_type=jnp.float32)
        rounded = lax.optimization_barrier(partial_value.astype(jnp.bfloat16))
        return (accum + rounded.astype(jnp.float32), None)
    accum, _ = lax.scan(add_group, jnp.zeros((TOKENS, D), jnp.float32), jnp.arange(N_TP, dtype=jnp.int32))
    return (accum.astype(jnp.bfloat16), log_totals)
```

```python
import functools

import jax
import jax.numpy as jnp
from jax import lax
from jax.experimental import pallas as pl
from jax.experimental.pallas import tpu as pltpu
from jax.sharding import PartitionSpec as P

LOG2E = 1.4426950408889634
LN2 = 0.6931471805599453
HIDDEN = -1e30


def project_kernel(place, own, other, gain, qw, kw, vw, gw, ow, iw, sw, kv, q, gate, outer, insig, normed):
    count, rows, part = own.shape
    width = normed.shape[1]

    def spread(core):
        squares = jnp.zeros((rows, part), jnp.float32)
        for x in range(count):
            for ref, side in ((own, core), (other, 1 - core)):
                at = (2 * x + side) * part
                piece = ref[x].astype(jnp.float32)
                squares = squares + piece * piece
                normed[:, at : at + part] = (piece * gain[:, at : at + part]).astype(jnp.bfloat16)
        scale = lax.rsqrt(jnp.sum(squares, axis=-1, keepdims=True) / width + 1e-06)

        def project(weight, factor=None):
            raw = jnp.dot(normed[...], weight[...], preferred_element_type=jnp.float32)
            raw = raw * scale
            if factor is not None:
                raw = raw * factor
            return raw.astype(jnp.bfloat16)

        columns = kw.shape[1]
        kv[:, :columns] = project(kw)
        kv[:, columns:] = project(vw)
        q[...] = project(qw, LOG2E * (columns // 2) ** -0.5)
        insig[...] = (project(iw).astype(jnp.float32) * project(sw).astype(jnp.float32)).astype(jnp.bfloat16)
        outer[...] = project(ow)
        gate[...] = project(gw)

    for core in range(2):
        pl.when(place[0] == core)(functools.partial(spread, core))


def attend_kernel(place, q, kv, out):
    rows = q.shape[1]
    blocks, block_len, columns = kv.shape
    value_size = columns // 2
    key_size = value_size // 2
    step = pl.program_id(0)
    last = place[0]
    slot = place[1]
    ahead = (step - slot) * rows
    queries = q[0]
    ones = jnp.ones((block_len, value_size), jnp.bfloat16)

    def body(used):
        stats = []
        for m in range(2):
            query = queries[:, m * key_size : (m + 1) * key_size]
            scores = []
            for b in range(used):
                keys = kv[b][:, m * key_size : (m + 1) * key_size]
                scores.append(
                    lax.dot_general(query, keys, (((1,), (1,)), ((), ())), preferred_element_type=jnp.float32)
                )
            row = lax.broadcasted_iota(jnp.int32, (rows, block_len), 0)
            col = lax.broadcasted_iota(jnp.int32, (rows, block_len), 1)
            seen = row + ahead >= col
            scores[-1] = jnp.where(seen, scores[-1], HIDDEN)
            top = scores[0]
            for s in scores[1:]:
                top = jnp.maximum(top, s)
            top = jnp.max(top, axis=-1, keepdims=True)
            summed = jnp.zeros((rows, 2 * value_size), jnp.float32)
            for b in range(used):
                w = jnp.exp2(scores[b] - top)
                if b == used - 1:
                    w = jnp.where(seen, w, 0.0)
                values = jnp.concatenate([kv[b][:, value_size:], ones], axis=1)
                summed = summed + jnp.dot(w.astype(jnp.bfloat16), values, preferred_element_type=jnp.float32)
            total = summed[:, value_size:]
            some = total > 0.0
            safe = jnp.where(some, total, 1.0)
            out[0, :rows, m * value_size : (m + 1) * value_size] = (summed[:, :value_size] / safe).astype(
                jnp.bfloat16
            )
            stats.append(jnp.where(some, jnp.log2(safe) + top, HIDDEN))
        lane = lax.broadcasted_iota(jnp.int32, (rows, value_size), 1)
        spread = jnp.zeros((rows, value_size), jnp.float32)
        for m in range(2):
            rest = stats[m]
            for piece in range(3):
                rounded = rest.astype(jnp.bfloat16).astype(jnp.float32)
                spread = jnp.where(lane == 2 * piece + m, rounded, spread)
                rest = rest - rounded
        turned = jnp.transpose(spread)
        out[0, rows:, :] = turned[: out.shape[1] - rows].astype(jnp.bfloat16)

    for used in range(1, blocks + 1):
        pl.when(last == used - 1)(functools.partial(body, used))


def finish_kernel(lam, parts, gate, conv, head_gain, attn_w, conv_w, mixed, totals):
    count, _, columns = parts.shape
    rows = gate.shape[0]
    value_size = columns // 2
    tails = [parts[j, rows:, :].astype(jnp.float32) for j in range(count)]
    logs = [t[0:2] + t[2:4] + t[4:6] for t in tails]
    top = logs[0]
    for log in logs[1:]:
        top = jnp.maximum(top, log)
    shares = [jnp.exp2(log - top) for log in logs]
    total = shares[0]
    for share in shares[1:]:
        total = total + share
    totals[0] = (jnp.log2(total) + top) * LN2
    shares = [share / total for share in shares]
    pad = jnp.zeros((value_size - 2 * count, rows), jnp.float32)
    turned = jnp.transpose(jnp.concatenate([*shares, pad], axis=0))
    mapped = []
    for m in range(2):
        summed = jnp.zeros((rows, value_size), jnp.float32)
        for j in range(count):
            piece = parts[j, :rows, m * value_size : (m + 1) * value_size].astype(jnp.float32)
            summed = summed + turned[:, 2 * j + m : 2 * j + m + 1] * piece
        mapped.append(summed)
    diff = mapped[0] - lam[0] * mapped[1]
    norm = lax.rsqrt(jnp.mean(diff * diff, axis=-1, keepdims=True) + 1e-05)
    opened = gate[...].astype(jnp.float32)
    head = diff * norm * head_gain[...] * (opened / (1.0 + jnp.exp(-opened)))
    mixed[...] = (
        jnp.dot(head.astype(jnp.bfloat16), attn_w[...], preferred_element_type=jnp.float32)
        + jnp.dot(conv[...], conv_w[...], preferred_element_type=jnp.float32)
    ).astype(jnp.bfloat16)


VMEM = pl.BlockSpec(memory_space=pltpu.VMEM)
SMEM = pl.BlockSpec(memory_space=pltpu.SMEM)


def project(core, own, other, gain, weights):
    rows = own.shape[1]
    width = gain.shape[0]
    columns = weights[0].shape[1]
    narrow = jax.ShapeDtypeStruct((rows, columns), jnp.bfloat16)
    return pl.pallas_call(
        project_kernel,
        out_shape=(jax.ShapeDtypeStruct((rows, 2 * columns), jnp.bfloat16), narrow, narrow, narrow, narrow),
        in_specs=[SMEM] + [VMEM] * 10,
        out_specs=(VMEM,) * 5,
        scratch_shapes=[pltpu.VMEM((rows, width), jnp.bfloat16)],
        name="project",
    )(core.reshape(1), own, other, gain.reshape(1, width), *weights)


def attend(place, queries, kv, extra):
    count, rows, columns = queries.shape
    return pl.pallas_call(
        attend_kernel,
        grid=(count,),
        out_shape=jax.ShapeDtypeStruct((count, rows + extra, kv.shape[2]), jnp.bfloat16),
        in_specs=[SMEM, pl.BlockSpec((1, rows, columns), lambda i: (i, 0, 0)), VMEM],
        out_specs=pl.BlockSpec((1, rows + extra, kv.shape[2]), lambda i: (i, 0, 0)),
        name="attend",
    )(place, queries, kv)


def finish(lambdas, parts, gate, conv, head_gain, attn_w, conv_w):
    rows = gate.shape[0]
    return pl.pallas_call(
        finish_kernel,
        out_shape=(
            jax.ShapeDtypeStruct((rows, attn_w.shape[1]), jnp.bfloat16),
            jax.ShapeDtypeStruct((1, 2, rows), jnp.float32),
        ),
        in_specs=[SMEM] + [VMEM] * 6,
        out_specs=(VMEM, VMEM),
        name="finish",
    )(lambdas, parts, gate, conv, head_gain.reshape(1, -1), attn_w, conv_w)


def convolve(outer, insig, taps):
    rows = insig.shape[0]
    reach = taps.shape[0] - 1
    count = lax.axis_size("sp")
    before = lax.ppermute(insig[rows - reach :], "sp", [(i, i + 1) for i in range(count - 1)])
    extended = jnp.concatenate([before, insig], axis=0).astype(jnp.float32)
    summed = jnp.zeros(insig.shape, jnp.float32)
    for j in range(reach + 1):
        summed = summed + taps[j] * extended[j : j + rows]
    return (outer.astype(jnp.float32) * summed).astype(jnp.bfloat16)


def per_device(
    tokens,
    norm_gain,
    query_weight,
    key_weight,
    value_weight,
    gate_weight,
    outer_weight,
    inner_weight,
    signal_weight,
    conv_taps,
    lambdas,
    head_gain,
    attn_out_weight,
    conv_out_weight,
):
    chunk = 8
    tp = lax.axis_size("tp")
    sp = lax.axis_size("sp")
    near = [[g * chunk + i for i in range(chunk)] for g in range(sp // chunk)]
    far = [[g * chunk + i for g in range(sp // chunk)] for i in range(chunk)]
    same_core = [[2 * x + c for x in range(tp // 2)] for c in range(2)]
    core = lax.rem(lax.axis_index("tp"), 2)
    index = lax.axis_index("sp")

    own = lax.all_gather(tokens, "tp", axis_index_groups=same_core)
    other = lax.ppermute(own, "tp", [(i, i ^ 1) for i in range(tp)])
    kv, query, gate, outer, insig = project(
        core,
        own,
        other,
        norm_gain,
        (query_weight, key_weight, value_weight, gate_weight, outer_weight, inner_weight, signal_weight),
    )
    all_kv = lax.all_gather(kv, "sp", axis_index_groups=far)
    queries = lax.all_gather(query, "sp", axis_index_groups=near)
    conv = convolve(outer, insig, conv_taps)
    place = jnp.stack([lax.div(index, chunk), lax.rem(index, chunk)]).astype(jnp.int32)
    parts = attend(place, queries, all_kv, 16)
    parts = lax.all_to_all(parts, "sp", 0, 0, axis_index_groups=near, tiled=True)
    partial, log_totals = finish(lambdas, parts, gate, conv, head_gain, attn_out_weight, conv_out_weight)
    tiles = lax.all_to_all(partial.reshape(tp, -1, partial.shape[1]), "tp", 0, 0, tiled=True)
    mixed = jnp.sum(tiles.astype(jnp.float32), axis=0).astype(jnp.bfloat16)
    return mixed, log_totals


def solution(mesh):
    placed = (
        P("sp", "tp"),
        P(),
        P(None, "tp"),
        P(None, "tp"),
        P(None, "tp"),
        P(None, "tp"),
        P(None, "tp"),
        P(None, "tp"),
        P(None, "tp"),
        P(None, "tp"),
        P("tp"),
        P("tp"),
        P("tp", None),
        P("tp", None),
    )
    return jax.shard_map(
        per_device,
        mesh=mesh,
        in_specs=placed,
        out_specs=(P(("sp", "tp"), None), P("tp", None, "sp")),
        check_vma=False,
    )
```

```python
import functools

import jax
import jax.numpy as jnp
from jax import lax
from jax.experimental import pallas as pl
from jax.experimental.pallas import tpu as pltpu
from jax.sharding import PartitionSpec as P

LOG2E = 1.4426950408889634
LN2 = 0.6931471805599453
HIDDEN = -1e30


def project_kernel(place, own, other, gain, qw, kw, vw, gw, ow, iw, sw, kv, q, gate, outer, insig, normed):
    count, rows, part = own.shape
    width = normed.shape[1]

    def spread(core):
        squares = jnp.zeros((rows, part), jnp.float32)
        for x in range(count):
            for ref, side in ((own, core), (other, 1 - core)):
                at = (2 * x + side) * part
                piece = ref[x].astype(jnp.float32)
                squares = squares + piece * piece
                normed[:, at : at + part] = (piece * gain[:, at : at + part]).astype(jnp.bfloat16)
        scale = lax.rsqrt(jnp.sum(squares, axis=-1, keepdims=True) / width + 1e-06)

        def project(weight, factor=None):
            raw = jnp.dot(normed[...], weight[...], preferred_element_type=jnp.float32)
            raw = raw * scale
            if factor is not None:
                raw = raw * factor
            return raw.astype(jnp.bfloat16)

        columns = kw.shape[1]
        kv[:, :columns] = project(kw)
        kv[:, columns:] = project(vw)
        query = project(qw, LOG2E * (columns // 2) ** -0.5)
        for i in range(q.shape[0]):
            q[i] = query
        insig[...] = (project(iw).astype(jnp.float32) * project(sw).astype(jnp.float32)).astype(jnp.bfloat16)
        outer[...] = project(ow)
        gate[...] = project(gw)

    for core in range(2):
        pl.when(place[0] == core)(functools.partial(spread, core))


def attend_kernel(place, q, *refs):
    blocks, out = refs[:-1], refs[-1]
    rows = q.shape[1]
    columns = blocks[0].shape[1]
    half = len(blocks) // 2
    value_size = columns // 2
    key_size = value_size // 2
    last = place[0]
    slot = place[1]
    ahead = (pl.program_id(0) - slot) * rows
    queries = q[0]

    def body(used):
        chosen = blocks[1:used] if used <= half else blocks[1 : used + 1]
        chosen = (*chosen, blocks[0])
        stats = []
        for m in range(2):
            query = queries[:, m * key_size : (m + 1) * key_size]
            scores = []
            for ref in chosen:
                keys = ref[:, m * key_size : (m + 1) * key_size]
                scores.append(
                    lax.dot_general(query, keys, (((1,), (1,)), ((), ())), preferred_element_type=jnp.float32)
                )
            row = lax.broadcasted_iota(jnp.int32, (rows, rows), 0)
            col = lax.broadcasted_iota(jnp.int32, (rows, rows), 1)
            seen = row + ahead >= col
            scores[-1] = jnp.where(seen, scores[-1], HIDDEN)
            tops = [s[:, i : i + value_size] for s in scores for i in range(0, s.shape[1], value_size)]
            top = tops[0]
            for s in tops[1:]:
                top = jnp.maximum(top, s)
            top = jnp.max(top, axis=-1, keepdims=True)
            summed = jnp.zeros((rows, 2 * value_size), jnp.float32)
            for ref, score in zip(chosen, scores):
                w = jnp.exp2(score - top)
                if ref is blocks[0]:
                    w = jnp.where(seen, w, 0.0)
                ones = jnp.ones((ref.shape[0], value_size), jnp.bfloat16)
                values = jnp.concatenate([ref[:, value_size:], ones], axis=1)
                summed = summed + jnp.dot(w.astype(jnp.bfloat16), values, preferred_element_type=jnp.float32)
            total = summed[:, value_size:]
            some = total > 0.0
            safe = jnp.where(some, total, 1.0)
            out[0, :rows, m * value_size : (m + 1) * value_size] = (summed[:, :value_size] / safe).astype(
                jnp.bfloat16
            )
            stats.append(jnp.where(some, jnp.log2(safe) + top, HIDDEN))
        lane = lax.broadcasted_iota(jnp.int32, (rows, value_size), 1)
        spread = jnp.zeros((rows, value_size), jnp.float32)
        for m in range(2):
            rest = stats[m]
            for piece in range(3):
                rounded = rest.astype(jnp.bfloat16).astype(jnp.float32)
                spread = jnp.where(lane == 2 * piece + m, rounded, spread)
                rest = rest - rounded
        turned = jnp.transpose(spread)
        out[0, rows:, :] = turned[: out.shape[1] - rows].astype(jnp.bfloat16)

    for used in range(1, len(blocks)):
        pl.when(last == used - 1)(functools.partial(body, used))


def finish_kernel(lam, parts, gate, conv, head_gain, attn_w, conv_w, mixed, totals):
    count, _, columns = parts.shape
    rows = gate.shape[0]
    value_size = columns // 2
    tails = [parts[j, rows:, :].astype(jnp.float32) for j in range(count)]
    logs = [t[0:2] + t[2:4] + t[4:6] for t in tails]
    top = logs[0]
    for log in logs[1:]:
        top = jnp.maximum(top, log)
    shares = [jnp.exp2(log - top) for log in logs]
    total = shares[0]
    for share in shares[1:]:
        total = total + share
    totals[0] = (jnp.log2(total) + top) * LN2
    shares = [share / total for share in shares]
    pad = jnp.zeros((value_size - 2 * count, rows), jnp.float32)
    turned = jnp.transpose(jnp.concatenate([*shares, pad], axis=0))
    mapped = []
    for m in range(2):
        summed = jnp.zeros((rows, value_size), jnp.float32)
        for j in range(count):
            piece = parts[j, :rows, m * value_size : (m + 1) * value_size].astype(jnp.float32)
            summed = summed + turned[:, 2 * j + m : 2 * j + m + 1] * piece
        mapped.append(summed)
    diff = mapped[0] - lam[0] * mapped[1]
    norm = lax.rsqrt(jnp.mean(diff * diff, axis=-1, keepdims=True) + 1e-05)
    opened = gate[...].astype(jnp.float32)
    head = diff * norm * head_gain[...] * (opened / (1.0 + jnp.exp(-opened)))
    mixed[...] = (
        jnp.dot(head.astype(jnp.bfloat16), attn_w[...], preferred_element_type=jnp.float32)
        + jnp.dot(conv[...], conv_w[...], preferred_element_type=jnp.float32)
    ).astype(jnp.bfloat16)


VMEM = pl.BlockSpec(memory_space=pltpu.VMEM)
SMEM = pl.BlockSpec(memory_space=pltpu.SMEM)


def project(core, own, other, gain, weights, copies):
    rows = own.shape[1]
    width = gain.shape[0]
    columns = weights[0].shape[1]
    narrow = jax.ShapeDtypeStruct((rows, columns), jnp.bfloat16)
    return pl.pallas_call(
        project_kernel,
        out_shape=(
            jax.ShapeDtypeStruct((rows, 2 * columns), jnp.bfloat16),
            jax.ShapeDtypeStruct((copies, rows, columns), jnp.bfloat16),
            narrow,
            narrow,
            narrow,
        ),
        in_specs=[SMEM] + [VMEM] * 10,
        out_specs=(VMEM,) * 5,
        scratch_shapes=[pltpu.VMEM((rows, width), jnp.bfloat16)],
        name="project",
    )(core.reshape(1), own, other, gain.reshape(1, width), *weights)


def attend(place, queries, blocks, extra):
    count, rows, columns = queries.shape
    wide = blocks[0].shape[1]
    return pl.pallas_call(
        attend_kernel,
        grid=(count,),
        out_shape=jax.ShapeDtypeStruct((count, rows + extra, wide), jnp.bfloat16),
        in_specs=[SMEM, pl.BlockSpec((1, rows, columns), lambda i: (i, 0, 0))] + [VMEM] * len(blocks),
        out_specs=pl.BlockSpec((1, rows + extra, wide), lambda i: (i, 0, 0)),
        name="attend",
    )(place, queries, *blocks)


def finish(lambdas, parts, gate, conv, head_gain, attn_w, conv_w):
    rows = gate.shape[0]
    return pl.pallas_call(
        finish_kernel,
        out_shape=(
            jax.ShapeDtypeStruct((rows, attn_w.shape[1]), jnp.bfloat16),
            jax.ShapeDtypeStruct((1, 2, rows), jnp.float32),
        ),
        in_specs=[SMEM] + [VMEM] * 6,
        out_specs=(VMEM, VMEM),
        name="finish",
    )(lambdas, parts, gate, conv, head_gain.reshape(1, -1), attn_w, conv_w)


def around(block, chunk):
    devices = lax.axis_size("sp")
    count = devices // chunk
    half = block.shape[0] // 2

    def moved(array, by):
        return lax.ppermute(array, "sp", [(i, (i + by * chunk) % devices) for i in range(devices)])

    ups, downs = [block], [block]
    for _ in range(count // 2 - 1):
        ups.append(moved(ups[-1], 1))
        downs.append(moved(downs[-1], -1))
    ups.append(moved(ups[-1][:half], 1))
    downs.append(moved(downs[-1][half:], -1))
    return ups + downs[:0:-1]


def convolve(outer, insig, taps):
    rows = insig.shape[0]
    reach = taps.shape[0] - 1
    count = lax.axis_size("sp")
    before = lax.ppermute(insig[rows - reach :], "sp", [(i, i + 1) for i in range(count - 1)])
    extended = jnp.concatenate([before, insig], axis=0).astype(jnp.float32)
    summed = jnp.zeros(insig.shape, jnp.float32)
    for j in range(reach + 1):
        summed = summed + taps[j] * extended[j : j + rows]
    return (outer.astype(jnp.float32) * summed).astype(jnp.bfloat16)


def per_device(
    tokens,
    norm_gain,
    query_weight,
    key_weight,
    value_weight,
    gate_weight,
    outer_weight,
    inner_weight,
    signal_weight,
    conv_taps,
    lambdas,
    head_gain,
    attn_out_weight,
    conv_out_weight,
):
    chunk = 8
    tp = lax.axis_size("tp")
    sp = lax.axis_size("sp")
    near = [[g * chunk + i for i in range(chunk)] for g in range(sp // chunk)]
    same_core = [[2 * x + c for x in range(tp // 2)] for c in range(2)]
    core = lax.rem(lax.axis_index("tp"), 2)
    index = lax.axis_index("sp")

    own = lax.all_gather(tokens, "tp", axis_index_groups=same_core)
    other = lax.ppermute(own, "tp", [(i, i ^ 1) for i in range(tp)])
    kv, query, gate, outer, insig = project(
        core,
        own,
        other,
        norm_gain,
        (query_weight, key_weight, value_weight, gate_weight, outer_weight, inner_weight, signal_weight),
        chunk,
    )
    queries = lax.all_to_all(query, "sp", 0, 0, axis_index_groups=near, tiled=True)
    blocks = around(kv, chunk)
    conv = convolve(outer, insig, conv_taps)
    place = jnp.stack([lax.div(index, chunk), lax.rem(index, chunk)]).astype(jnp.int32)
    parts = attend(place, queries, blocks, 16)
    parts = lax.all_to_all(parts, "sp", 0, 0, axis_index_groups=near, tiled=True)
    partial, log_totals = finish(lambdas, parts, gate, conv, head_gain, attn_out_weight, conv_out_weight)
    tiles = lax.all_to_all(partial.reshape(tp, -1, partial.shape[1]), "tp", 0, 0, tiled=True)
    mixed = jnp.sum(tiles.astype(jnp.float32), axis=0).astype(jnp.bfloat16)
    return mixed, log_totals


def solution(mesh):
    placed = (
        P("sp", "tp"),
        P(),
        P(None, "tp"),
        P(None, "tp"),
        P(None, "tp"),
        P(None, "tp"),
        P(None, "tp"),
        P(None, "tp"),
        P(None, "tp"),
        P(None, "tp"),
        P("tp"),
        P("tp"),
        P("tp", None),
        P("tp", None),
    )
    return jax.shard_map(
        per_device,
        mesh=mesh,
        in_specs=placed,
        out_specs=(P(("sp", "tp"), None), P("tp", None, "sp")),
        check_vma=False,
    )
```

```python
import functools

import jax
import jax.numpy as jnp
from jax import lax
from jax.experimental import pallas as pl
from jax.experimental.pallas import tpu as pltpu
from jax.sharding import PartitionSpec as P

LOG2E = 1.4426950408889634
LN2 = 0.6931471805599453
HIDDEN = -1e30


def project_kernel(own, other, gain, qw, kw, vw, gw, ow, iw, sw, kv, q, gate, outer, insig, normed):
    count, rows, part = own.shape
    width = normed.shape[1]

    def spread(core):
        squares = jnp.zeros((rows, part), jnp.float32)
        for x in range(count):
            for ref, side in ((own, core), (other, 1 - core)):
                at = (2 * x + side) * part
                piece = ref[x].astype(jnp.float32)
                squares = squares + piece * piece
                normed[:, at : at + part] = (piece * gain[:, at : at + part]).astype(jnp.bfloat16)
        scale = lax.rsqrt(jnp.sum(squares, axis=-1, keepdims=True) / width + 1e-06)

        def project(weight, factor=None):
            raw = jnp.dot(normed[...], weight[...], preferred_element_type=jnp.float32)
            raw = raw * scale
            if factor is not None:
                raw = raw * factor
            return raw.astype(jnp.bfloat16)

        columns = kw.shape[1]
        kv[:, :columns] = project(kw)
        kv[:, columns:] = project(vw)
        query = project(qw, LOG2E * (columns // 2) ** -0.5)
        for i in range(q.shape[0]):
            q[i] = query
        insig[...] = (project(iw).astype(jnp.float32) * project(sw).astype(jnp.float32)).astype(jnp.bfloat16)
        outer[...] = project(ow)
        gate[...] = project(gw)

    for core in range(2):
        pl.when(lax.rem(lax.axis_index("tp"), 2) == core)(functools.partial(spread, core))


def attend_kernel(chunk, span, q, own, kv, out, held):
    rows = q.shape[1]
    columns = kv.shape[2]
    value_size = columns // 2
    key_size = value_size // 2
    index = lax.axis_index("sp")
    last = lax.div(index, chunk)
    slot = lax.rem(index, chunk)
    first = pl.program_id(0) * span
    lane = lax.broadcasted_iota(jnp.int32, (rows, value_size), 1)
    units = [(i, m) for i in range(span) for m in range(2)]

    def body(full):
        order = [*range(full), None]
        ones = jnp.ones((rows, value_size), jnp.bfloat16)
        row = lax.broadcasted_iota(jnp.int32, (rows, rows), 0)
        col = lax.broadcasted_iota(jnp.int32, (rows, rows), 1)

        def part(b, cut):
            return own[:, cut] if b is None else kv[b, :, cut]

        def seen(i):
            return row + (first + i - slot) * rows >= col

        def score(u, b):
            i, m = units[u]
            cut = slice(m * key_size, (m + 1) * key_size)
            s = lax.dot_general(
                q[i, :, cut], part(b, cut), (((1,), (1,)), ((), ())), preferred_element_type=jnp.float32
            )
            if b is None:
                s = jnp.where(seen(i), s, HIDDEN)
            held[u % 2, full if b is None else b] = s
            top = s[:, :value_size]
            for at in range(value_size, rows, value_size):
                top = jnp.maximum(top, s[:, at : at + value_size])
            return top

        def peak(tops):
            top = tops[0]
            for t in tops[1:]:
                top = jnp.maximum(top, t)
            return jnp.max(top, axis=-1, keepdims=True)

        stats = []
        top = peak([score(0, b) for b in order])
        for u, (i, m) in enumerate(units):
            ahead = []
            summed = jnp.zeros((rows, 2 * value_size), jnp.float32)
            for b in order:
                if u + 1 < len(units):
                    ahead.append(score(u + 1, b))
                w = jnp.exp2(held[u % 2, full if b is None else b] - top)
                if b is None:
                    w = jnp.where(seen(i), w, 0.0)
                values = jnp.concatenate([part(b, slice(value_size, None)), ones], axis=1)
                summed = summed + jnp.dot(w.astype(jnp.bfloat16), values, preferred_element_type=jnp.float32)
            total = summed[:, value_size:]
            some = total > 0.0
            safe = jnp.where(some, total, 1.0)
            out[i, :rows, m * value_size : (m + 1) * value_size] = (summed[:, :value_size] / safe).astype(
                jnp.bfloat16
            )
            stats.append(jnp.where(some, jnp.log2(safe) + top, HIDDEN))
            if ahead:
                top = peak(ahead)
        for i in range(span):
            spread = jnp.zeros((rows, value_size), jnp.float32)
            for m in range(2):
                rest = stats[2 * i + m]
                for piece in range(3):
                    rounded = rest.astype(jnp.bfloat16).astype(jnp.float32)
                    spread = jnp.where(lane == 2 * piece + m, rounded, spread)
                    rest = rest - rounded
            turned = jnp.transpose(spread)
            out[i, rows:, :] = turned[: out.shape[1] - rows].astype(jnp.bfloat16)

    for full in range(kv.shape[0] + 1):
        pl.when(last == full)(functools.partial(body, full))


def finish_kernel(lam, parts, gate, conv, head_gain, attn_w, conv_w, mixed, totals):
    count, _, columns = parts.shape
    rows = gate.shape[0]
    value_size = columns // 2
    tails = [parts[j, rows:, :].astype(jnp.float32) for j in range(count)]
    logs = [t[0:2] + t[2:4] + t[4:6] for t in tails]
    top = logs[0]
    for log in logs[1:]:
        top = jnp.maximum(top, log)
    shares = [jnp.exp2(log - top) for log in logs]
    total = shares[0]
    for share in shares[1:]:
        total = total + share
    totals[0] = (jnp.log2(total) + top) * LN2
    shares = [share / total for share in shares]
    pad = jnp.zeros((value_size - 2 * count, rows), jnp.float32)
    turned = jnp.transpose(jnp.concatenate([*shares, pad], axis=0))
    mapped = []
    for m in range(2):
        summed = jnp.zeros((rows, value_size), jnp.float32)
        for j in range(count):
            piece = parts[j, :rows, m * value_size : (m + 1) * value_size].astype(jnp.float32)
            summed = summed + turned[:, 2 * j + m : 2 * j + m + 1] * piece
        mapped.append(summed)
    diff = mapped[0] - lam[0] * mapped[1]
    norm = lax.rsqrt(jnp.mean(diff * diff, axis=-1, keepdims=True) + 1e-05)
    opened = gate[...].astype(jnp.float32)
    head = diff * norm * head_gain[...] * (opened / (1.0 + jnp.exp(-opened)))
    mixed[...] = (
        jnp.dot(head.astype(jnp.bfloat16), attn_w[...], preferred_element_type=jnp.float32)
        + jnp.dot(conv[...], conv_w[...], preferred_element_type=jnp.float32)
    ).astype(jnp.bfloat16)


VMEM = pl.BlockSpec(memory_space=pltpu.VMEM)
SMEM = pl.BlockSpec(memory_space=pltpu.SMEM)


def project(own, other, gain, weights, copies):
    rows = own.shape[1]
    width = gain.shape[0]
    columns = weights[0].shape[1]
    narrow = jax.ShapeDtypeStruct((rows, columns), jnp.bfloat16)
    return pl.pallas_call(
        project_kernel,
        out_shape=(
            jax.ShapeDtypeStruct((rows, 2 * columns), jnp.bfloat16),
            jax.ShapeDtypeStruct((copies, rows, columns), jnp.bfloat16),
            narrow,
            narrow,
            narrow,
        ),
        in_specs=[VMEM] * 10,
        out_specs=(VMEM,) * 5,
        scratch_shapes=[pltpu.VMEM((rows, width), jnp.bfloat16)],
        name="project",
    )(own, other, gain.reshape(1, width), *weights)


def attend(queries, own, kv, chunk, extra):
    count, rows, columns = queries.shape
    others, _, wide = kv.shape
    span = 2

    def tiled(length, width):
        return pl.BlockSpec((span, length, width), lambda i: (i, 0, 0))

    return pl.pallas_call(
        functools.partial(attend_kernel, chunk, span),
        grid=(count // span,),
        out_shape=jax.ShapeDtypeStruct((count, rows + extra, wide), jnp.bfloat16),
        in_specs=[tiled(rows, columns), VMEM, VMEM],
        out_specs=tiled(rows + extra, wide),
        scratch_shapes=[pltpu.VMEM((2, others + 1, rows, rows), jnp.float32)],
        name="attend",
    )(queries, own, kv)


def finish(lambdas, parts, gate, conv, head_gain, attn_w, conv_w):
    rows = gate.shape[0]
    return pl.pallas_call(
        finish_kernel,
        out_shape=(
            jax.ShapeDtypeStruct((rows, attn_w.shape[1]), jnp.bfloat16),
            jax.ShapeDtypeStruct((1, 2, rows), jnp.float32),
        ),
        in_specs=[SMEM] + [VMEM] * 6,
        out_specs=(VMEM, VMEM),
        name="finish",
    )(lambdas, parts, gate, conv, head_gain.reshape(1, -1), attn_w, conv_w)


def earlier_blocks(block, groups, chunk):
    devices = lax.axis_size("sp")
    count = devices // chunk
    rows, wide = block.shape
    step = rows // count
    share = rows - step
    before = lax.ppermute(block[step:], "sp", [(i, i + chunk) for i in range(devices - chunk)])
    start = share - lax.div(lax.axis_index("sp"), chunk) * step
    held = lax.dynamic_slice_in_dim(jnp.concatenate([before, block], axis=0), start, share, 0)
    gathered = lax.all_gather(held, "sp", axis_index_groups=groups, tiled=True)
    return gathered.reshape(count - 1, rows, wide)


def convolve(outer, insig, taps):
    rows = insig.shape[0]
    reach = taps.shape[0] - 1
    count = lax.axis_size("sp")
    before = lax.ppermute(insig[rows - reach :], "sp", [(i, i + 1) for i in range(count - 1)])
    extended = jnp.concatenate([before, insig], axis=0).astype(jnp.float32)
    summed = jnp.zeros(insig.shape, jnp.float32)
    for j in range(reach + 1):
        summed = summed + taps[j] * extended[j : j + rows]
    return (outer.astype(jnp.float32) * summed).astype(jnp.bfloat16)


def per_device(
    tokens,
    norm_gain,
    query_weight,
    key_weight,
    value_weight,
    gate_weight,
    outer_weight,
    inner_weight,
    signal_weight,
    conv_taps,
    lambdas,
    head_gain,
    attn_out_weight,
    conv_out_weight,
):
    chunk = 8
    tp = lax.axis_size("tp")
    sp = lax.axis_size("sp")
    near = [[g * chunk + i for i in range(chunk)] for g in range(sp // chunk)]
    far = [[g * chunk + i for g in range(sp // chunk)] for i in range(chunk)]
    same_core = [[2 * x + c for x in range(tp // 2)] for c in range(2)]

    own = lax.all_gather(tokens, "tp", axis_index_groups=same_core)
    other = lax.ppermute(own, "tp", [(i, i ^ 1) for i in range(tp)])
    kv, query, gate, outer, insig = project(
        own,
        other,
        norm_gain,
        (query_weight, key_weight, value_weight, gate_weight, outer_weight, inner_weight, signal_weight),
        chunk,
    )
    queries = lax.all_to_all(query, "sp", 0, 0, axis_index_groups=near, tiled=True)
    conv = convolve(outer, insig, conv_taps)
    parts = attend(queries, kv, earlier_blocks(kv, far, chunk), chunk, 16)
    parts = lax.all_to_all(parts, "sp", 0, 0, axis_index_groups=near, tiled=True)
    partial, log_totals = finish(lambdas, parts, gate, conv, head_gain, attn_out_weight, conv_out_weight)
    tiles = lax.all_to_all(partial.reshape(tp, -1, partial.shape[1]), "tp", 0, 0, tiled=True)
    mixed = jnp.sum(tiles.astype(jnp.float32), axis=0).astype(jnp.bfloat16)
    return mixed, log_totals


def solution(mesh):
    placed = (
        P("sp", "tp"),
        P(),
        P(None, "tp"),
        P(None, "tp"),
        P(None, "tp"),
        P(None, "tp"),
        P(None, "tp"),
        P(None, "tp"),
        P(None, "tp"),
        P(None, "tp"),
        P("tp"),
        P("tp"),
        P("tp", None),
        P("tp", None),
    )
    return jax.shard_map(
        per_device,
        mesh=mesh,
        in_specs=placed,
        out_specs=(P(("sp", "tp"), None), P("tp", None, "sp")),
        check_vma=False,
    )
```

```python
import functools

import jax
import jax.numpy as jnp
from jax import lax
from jax.experimental import pallas as pl
from jax.experimental.pallas import tpu as pltpu
from jax.sharding import PartitionSpec as P


LOG2E = 1.4426950408889634
LN2 = 0.6931471805599453
HIDDEN = -1e30


def project_kernel(own, other, gain, qw, kw, vw, iw, sw, kv, q, normed, scaled):
    count, rows, part = own.shape
    width = normed.shape[1]
    tail = kv.shape[0] - rows

    def spread(core):
        squares = jnp.zeros((rows, part), jnp.float32)
        for x in range(count):
            for ref, side in ((own, core), (other, 1 - core)):
                at = (2 * x + side) * part
                piece = ref[x].astype(jnp.float32)
                squares = squares + piece * piece
                normed[:, at : at + part] = (piece * gain[:, at : at + part]).astype(jnp.bfloat16)
        scale = lax.rsqrt(jnp.sum(squares, axis=-1, keepdims=True) / width + 1e-06)

        def project(weight, low=0, factor=None):
            raw = jnp.dot(normed[low:, :], weight[...], preferred_element_type=jnp.float32)
            raw = raw * scale[low:]
            if factor is not None:
                raw = raw * factor
            return raw.astype(jnp.bfloat16)

        columns = kw.shape[1]
        kv[:rows, :columns] = project(kw)
        kv[:rows, columns:] = project(vw)
        low = rows - tail
        ending = project(iw, low).astype(jnp.float32) * project(sw, low).astype(jnp.float32)
        kv[rows:, :columns] = ending.astype(jnp.bfloat16)
        kv[rows:, columns:] = jnp.zeros((tail, columns), jnp.bfloat16)
        query = project(qw, 0, LOG2E * (columns // 2) ** -0.5)
        for i in range(q.shape[0]):
            q[i] = query
        scaled[...] = jnp.broadcast_to(scale, scaled.shape)

    for core in range(2):
        pl.when(lax.rem(lax.axis_index("tp"), 2) == core)(functools.partial(spread, core))


def gates_kernel(normed, scale, gw, ow, iw, sw, gate, outer, insig):
    def project(weight):
        raw = jnp.dot(normed[...], weight[...], preferred_element_type=jnp.float32)
        return (raw * scale[...]).astype(jnp.bfloat16)

    insig[...] = (project(iw).astype(jnp.float32) * project(sw).astype(jnp.float32)).astype(jnp.bfloat16)
    outer[...] = project(ow)
    gate[...] = project(gw)


def attend_kernel(chunk, span, q, own, kv, ending, out, held):
    rows = q.shape[1]
    columns = kv.shape[2]
    value_size = columns // 2
    key_size = value_size // 2
    index = lax.axis_index("sp")
    last = lax.div(index, chunk)
    slot = lax.rem(index, chunk)
    first = pl.program_id(0) * span
    lane = lax.broadcasted_iota(jnp.int32, (rows, value_size), 1)
    units = [(i, m) for i in range(span) for m in range(2)]

    def body(full):
        order = [*range(full), None]
        ones = jnp.ones((rows, value_size), jnp.bfloat16)
        row = lax.broadcasted_iota(jnp.int32, (rows, rows), 0)
        col = lax.broadcasted_iota(jnp.int32, (rows, rows), 1)

        def part(b, cut):
            return own[:rows, cut] if b is None else kv[b, :, cut]

        def seen(i):
            return row + (first + i - slot) * rows >= col

        def score(u, b):
            i, m = units[u]
            cut = slice(m * key_size, (m + 1) * key_size)
            s = lax.dot_general(
                q[i, :, cut], part(b, cut), (((1,), (1,)), ((), ())), preferred_element_type=jnp.float32
            )
            if b is None:
                s = jnp.where(seen(i), s, HIDDEN)
            held[u % 2, full if b is None else b] = s
            top = s[:, :value_size]
            for at in range(value_size, rows, value_size):
                top = jnp.maximum(top, s[:, at : at + value_size])
            return top

        def peak(tops):
            top = tops[0]
            for t in tops[1:]:
                top = jnp.maximum(top, t)
            return jnp.max(top, axis=-1, keepdims=True)

        stats = []
        top = peak([score(0, b) for b in order])
        for u, (i, m) in enumerate(units):
            ahead = []
            summed = jnp.zeros((rows, 2 * value_size), jnp.float32)
            for b in order:
                if u + 1 < len(units):
                    ahead.append(score(u + 1, b))
                w = jnp.exp2(held[u % 2, full if b is None else b] - top)
                if b is None:
                    w = jnp.where(seen(i), w, 0.0)
                values = jnp.concatenate([part(b, slice(value_size, None)), ones], axis=1)
                summed = summed + jnp.dot(w.astype(jnp.bfloat16), values, preferred_element_type=jnp.float32)
            total = summed[:, value_size:]
            some = total > 0.0
            safe = jnp.where(some, total, 1.0)
            out[i, :rows, m * value_size : (m + 1) * value_size] = (summed[:, :value_size] / safe).astype(
                jnp.bfloat16
            )
            stats.append(jnp.where(some, jnp.log2(safe) + top, HIDDEN))
            if ahead:
                top = peak(ahead)
        for i in range(span):
            spread = jnp.zeros((rows, value_size), jnp.float32)
            for m in range(2):
                rest = stats[2 * i + m]
                for piece in range(3):
                    rounded = rest.astype(jnp.bfloat16).astype(jnp.float32)
                    spread = jnp.where(lane == 2 * piece + m, rounded, spread)
                    rest = rest - rounded
            tail = out.shape[1] - rows
            turned = jnp.transpose(spread)[:tail].astype(jnp.bfloat16)
            ends = jnp.concatenate([own[rows:, :value_size], ending[:, :value_size]], axis=1)
            line = lax.broadcasted_iota(jnp.int32, (tail, columns), 0)
            out[i, rows:, :] = jnp.where(line < tail // 2, turned, ends)

    for full in range(kv.shape[0] + 1):
        pl.when(last == full)(functools.partial(body, full))


def finish_kernel(lam, parts, gate, outer, insig, taps, head_gain, attn_w, conv_w, mixed, totals):
    count, _, columns = parts.shape
    rows = gate.shape[0]
    value_size = columns // 2
    tails = [parts[j, rows:, :].astype(jnp.float32) for j in range(count)]
    logs = [t[0:2] + t[2:4] + t[4:6] for t in tails]
    top = logs[0]
    for log in logs[1:]:
        top = jnp.maximum(top, log)
    shares = [jnp.exp2(log - top) for log in logs]
    total = shares[0]
    for share in shares[1:]:
        total = total + share
    totals[0] = (jnp.log2(total) + top) * LN2
    shares = [share / total for share in shares]
    pad = jnp.zeros((value_size - 2 * count, rows), jnp.float32)
    turned = jnp.transpose(jnp.concatenate([*shares, pad], axis=0))
    mapped = []
    for m in range(2):
        summed = jnp.zeros((rows, value_size), jnp.float32)
        for j in range(count):
            piece = parts[j, :rows, m * value_size : (m + 1) * value_size].astype(jnp.float32)
            summed = summed + turned[:, 2 * j + m : 2 * j + m + 1] * piece
        mapped.append(summed)
    diff = mapped[0] - lam[0] * mapped[1]
    norm = lax.rsqrt(jnp.mean(diff * diff, axis=-1, keepdims=True) + 1e-05)
    opened = gate[...].astype(jnp.float32)
    head = diff * norm * head_gain[...] * (opened / (1.0 + jnp.exp(-opened)))
    slot = lax.rem(lax.axis_index("sp"), count)
    ends = parts[lax.rem(slot + count - 1, count), rows:, :].astype(jnp.float32)
    ends = jnp.where(slot == 0, ends[:, value_size:], ends[:, :value_size])
    reach = taps.shape[0] - 1
    signal = insig[...].astype(jnp.float32)
    row = lax.broadcasted_iota(jnp.int32, signal.shape, 0)
    convolved = taps[reach : reach + 1, :] * signal
    for by in range(1, reach + 1):
        moved = pltpu.roll(signal, by, axis=0)
        for at in range(by):
            line = ends.shape[0] - by + at
            moved = jnp.where(row == at, ends[line : line + 1, :], moved)
        convolved = convolved + taps[reach - by : reach - by + 1, :] * moved
    conv = (outer[...].astype(jnp.float32) * convolved).astype(jnp.bfloat16)
    mixed[...] = (
        jnp.dot(head.astype(jnp.bfloat16), attn_w[...], preferred_element_type=jnp.float32)
        + jnp.dot(conv, conv_w[...], preferred_element_type=jnp.float32)
    ).astype(jnp.bfloat16)


VMEM = pl.BlockSpec(memory_space=pltpu.VMEM)
SMEM = pl.BlockSpec(memory_space=pltpu.SMEM)


def project(own, other, gain, weights, copies, tail):
    rows = own.shape[1]
    width = gain.shape[0]
    columns = weights[0].shape[1]
    return pl.pallas_call(
        project_kernel,
        out_shape=(
            jax.ShapeDtypeStruct((rows + tail, 2 * columns), jnp.bfloat16),
            jax.ShapeDtypeStruct((copies, rows, columns), jnp.bfloat16),
            jax.ShapeDtypeStruct((rows, width), jnp.bfloat16),
            jax.ShapeDtypeStruct((rows, columns), jnp.float32),
        ),
        in_specs=[VMEM] * 8,
        out_specs=(VMEM,) * 4,
        name="project",
    )(own, other, gain.reshape(1, width), *weights)


def gates(normed, scale, weights):
    shape = jax.ShapeDtypeStruct((normed.shape[0], weights[0].shape[1]), jnp.bfloat16)
    return pl.pallas_call(
        gates_kernel,
        out_shape=(shape,) * 3,
        in_specs=[VMEM] * 6,
        out_specs=(VMEM,) * 3,
        cost_estimate=pl.CostEstimate(flops=8 * normed.size * weights[0].shape[1], transcendentals=0, bytes_accessed=4 * normed.size),
        name="gates",
    )(normed, scale, *weights)


def attend(queries, own, kv, ending, chunk):
    count, rows, columns = queries.shape
    others, _, wide = kv.shape
    extra = ending.shape[0]
    span = 2

    def tiled(length, width):
        return pl.BlockSpec((span, length, width), lambda i: (i, 0, 0))

    return pl.pallas_call(
        functools.partial(attend_kernel, chunk, span),
        grid=(count // span,),
        out_shape=jax.ShapeDtypeStruct((count, rows + extra, wide), jnp.bfloat16),
        in_specs=[tiled(rows, columns), VMEM, VMEM, VMEM],
        out_specs=tiled(rows + extra, wide),
        scratch_shapes=[pltpu.VMEM((2, others + 1, rows, rows), jnp.float32)],
        name="attend",
    )(queries, own, kv, ending)


def finish(lambdas, parts, gate, outer, insig, taps, head_gain, attn_w, conv_w):
    rows = gate.shape[0]
    return pl.pallas_call(
        finish_kernel,
        out_shape=(
            jax.ShapeDtypeStruct((rows, attn_w.shape[1]), jnp.bfloat16),
            jax.ShapeDtypeStruct((1, 2, rows), jnp.float32),
        ),
        in_specs=[SMEM] + [VMEM] * 8,
        out_specs=(VMEM, VMEM),
        name="finish",
    )(lambdas, parts, gate, outer, insig, taps, head_gain.reshape(1, -1), attn_w, conv_w)


def earlier_blocks(block, groups, chunk, tail):
    devices = lax.axis_size("sp")
    count = devices // chunk
    rows, wide = block.shape[0] - tail, block.shape[1]
    step = rows // count
    share = rows - step
    before = lax.ppermute(block[step:], "sp", [(i, i + chunk) for i in range(devices - chunk)])
    start = share - lax.div(lax.axis_index("sp"), chunk) * step
    held = lax.dynamic_slice_in_dim(jnp.concatenate([before[:share], block[:rows]], axis=0), start, share, 0)
    gathered = lax.all_gather(held, "sp", axis_index_groups=groups, tiled=True)
    return gathered.reshape(count - 1, rows, wide), before[share:]


def per_device(
    tokens,
    norm_gain,
    query_weight,
    key_weight,
    value_weight,
    gate_weight,
    outer_weight,
    inner_weight,
    signal_weight,
    conv_taps,
    lambdas,
    head_gain,
    attn_out_weight,
    conv_out_weight,
):
    chunk = 8
    tp = lax.axis_size("tp")
    sp = lax.axis_size("sp")
    near = [[g * chunk + i for i in range(chunk)] for g in range(sp // chunk)]
    far = [[g * chunk + i for g in range(sp // chunk)] for i in range(chunk)]
    same_core = [[2 * x + c for x in range(tp // 2)] for c in range(2)]

    own = lax.all_gather(tokens, "tp", axis_index_groups=same_core)
    other = lax.ppermute(own, "tp", [(i, i ^ 1) for i in range(tp)])
    tail = 16
    kv, query, normed, scale = project(
        own,
        other,
        norm_gain,
        (query_weight, key_weight, value_weight, inner_weight, signal_weight),
        chunk,
        tail,
    )
    queries = lax.all_to_all(query, "sp", 0, 0, axis_index_groups=near, tiled=True)
    earlier, ending = earlier_blocks(kv, far, chunk, tail)
    parts = attend(queries, kv, earlier, ending, chunk)
    normed, parts = lax.optimization_barrier((normed, parts))
    gate, outer, insig = gates(normed, scale, (gate_weight, outer_weight, inner_weight, signal_weight))
    parts = lax.all_to_all(parts, "sp", 0, 0, axis_index_groups=near, tiled=True)
    partial, log_totals = finish(
        lambdas, parts, gate, outer, insig, conv_taps, head_gain, attn_out_weight, conv_out_weight
    )
    tiles = lax.all_to_all(partial.reshape(tp, -1, partial.shape[1]), "tp", 0, 0, tiled=True)
    mixed = jnp.sum(tiles.astype(jnp.float32), axis=0).astype(jnp.bfloat16)
    return mixed, log_totals


def solution(mesh):
    placed = (
        P("sp", "tp"),
        P(),
        P(None, "tp"),
        P(None, "tp"),
        P(None, "tp"),
        P(None, "tp"),
        P(None, "tp"),
        P(None, "tp"),
        P(None, "tp"),
        P(None, "tp"),
        P("tp"),
        P("tp"),
        P("tp", None),
        P("tp", None),
    )

    return jax.shard_map(
        per_device,
        mesh=mesh,
        in_specs=placed,
        out_specs=(P(("sp", "tp"), None), P("tp", None, "sp")),
        check_vma=False,
    )
```

```python
import functools

import jax
import jax.numpy as jnp
from jax import lax
from jax.experimental import pallas as pl
from jax.experimental.pallas import tpu as pltpu
from jax.sharding import PartitionSpec as P


LOG2E = 1.4426950408889634
LN2 = 0.6931471805599453
HIDDEN = -1e30


def project_kernel(own, gain, qw, kw, vw, iw, sw, other, kv, shifted, q, normed, scaled):
    count, rows, part = own.shape
    width = normed.shape[1]
    skipped = rows // q.shape[0]
    tail = shifted.shape[0] + skipped - rows

    def spread(core):
        squares = jnp.zeros((rows, part), jnp.float32)
        for ref, side in ((own, core), (other, 1 - core)):
            for x in range(count):
                at = (2 * x + side) * part
                piece = ref[x].astype(jnp.float32)
                squares = squares + piece * piece
                normed[:, at : at + part] = (piece * gain[:, at : at + part]).astype(jnp.bfloat16)
        scale = lax.rsqrt(jnp.sum(squares, axis=-1, keepdims=True) / width + 1e-06)

        def project(weight, low=0, factor=None):
            raw = jnp.dot(normed[low:, :], weight[...], preferred_element_type=jnp.float32)
            raw = raw * scale[low:]
            if factor is not None:
                raw = raw * factor
            return raw.astype(jnp.bfloat16)

        columns = kw.shape[1]
        for n, weight in enumerate((kw, vw)):
            cut = slice(n * columns, (n + 1) * columns)
            values = project(weight)
            kv[:, cut] = values
            shifted[: rows - skipped, cut] = values[skipped:]
        low = rows - tail
        ending = project(iw, low).astype(jnp.float32) * project(sw, low).astype(jnp.float32)
        shifted[rows - skipped :, :columns] = ending.astype(jnp.bfloat16)
        shifted[rows - skipped :, columns:] = jnp.zeros((tail, columns), jnp.bfloat16)
        query = project(qw, 0, LOG2E * (columns // 2) ** -0.5)
        for i in range(q.shape[0]):
            q[i] = query
        scaled[...] = jnp.broadcast_to(scale, scaled.shape)

    for core in range(2):
        pl.when(lax.rem(lax.axis_index("tp"), 2) == core)(functools.partial(spread, core))


def gates_kernel(normed, scale, gw, ow, iw, sw, gate, outer, insig):
    def project(weight):
        raw = jnp.dot(normed[...], weight[...], preferred_element_type=jnp.float32)
        return (raw * scale[...]).astype(jnp.bfloat16)

    insig[...] = (project(iw).astype(jnp.float32) * project(sw).astype(jnp.float32)).astype(jnp.bfloat16)
    outer[...] = project(ow)
    gate[...] = project(gw)


def attend_kernel(chunk, span, q, own, ending, moved, kv, out, held):
    rows = q.shape[1]
    columns = kv.shape[2]
    value_size = columns // 2
    key_size = value_size // 2
    index = lax.axis_index("sp")
    last = lax.div(index, chunk)
    slot = lax.rem(index, chunk)
    first = pl.program_id(0) * span
    lane = lax.broadcasted_iota(jnp.int32, (rows, value_size), 1)
    units = [(i, m) for i in range(span) for m in range(2)]

    def body(full):
        order = [*range(full), None]
        ones = jnp.ones((rows, value_size), jnp.bfloat16)
        row = lax.broadcasted_iota(jnp.int32, (rows, rows), 0)
        col = lax.broadcasted_iota(jnp.int32, (rows, rows), 1)

        def part(b, cut):
            return own[:, cut] if b is None else kv[b, :, cut]

        def seen(i):
            return row + (first + i - slot) * rows >= col

        def score(u, b):
            i, m = units[u]
            cut = slice(m * key_size, (m + 1) * key_size)
            s = lax.dot_general(
                q[first + i, :, cut], part(b, cut), (((1,), (1,)), ((), ())), preferred_element_type=jnp.float32
            )
            if b is None:
                s = jnp.where(seen(i), s, HIDDEN)
            held[u % 2, full if b is None else b] = s
            top = s[:, :value_size]
            for at in range(value_size, rows, value_size):
                top = jnp.maximum(top, s[:, at : at + value_size])
            return top

        def peak(tops):
            top = tops[0]
            for t in tops[1:]:
                top = jnp.maximum(top, t)
            return jnp.max(top, axis=-1, keepdims=True)

        stats = []
        top = peak([score(0, b) for b in order])
        for u, (i, m) in enumerate(units):
            ahead = []
            summed = jnp.zeros((rows, 2 * value_size), jnp.float32)
            for b in order:
                if u + 1 < len(units):
                    ahead.append(score(u + 1, b))
                w = jnp.exp2(held[u % 2, full if b is None else b] - top)
                if b is None:
                    w = jnp.where(seen(i), w, 0.0)
                values = jnp.concatenate([part(b, slice(value_size, None)), ones], axis=1)
                summed = summed + jnp.dot(w.astype(jnp.bfloat16), values, preferred_element_type=jnp.float32)
            total = summed[:, value_size:]
            some = total > 0.0
            safe = jnp.where(some, total, 1.0)
            out[i, :rows, m * value_size : (m + 1) * value_size] = (summed[:, :value_size] / safe).astype(
                jnp.bfloat16
            )
            stats.append(jnp.where(some, jnp.log2(safe) + top, HIDDEN))
            if ahead:
                top = peak(ahead)
        for i in range(span):
            spread = jnp.zeros((rows, value_size), jnp.float32)
            for m in range(2):
                rest = stats[2 * i + m]
                for piece in range(3):
                    rounded = rest.astype(jnp.bfloat16).astype(jnp.float32)
                    spread = jnp.where(lane == 2 * piece + m, rounded, spread)
                    rest = rest - rounded
            tail = out.shape[1] - rows
            turned = jnp.transpose(spread)[:tail].astype(jnp.bfloat16)
            ends = [ref[ref.shape[0] - tail :, :value_size] for ref in (ending, moved)]
            ends = jnp.concatenate(ends, axis=1)
            line = lax.broadcasted_iota(jnp.int32, (tail, columns), 0)
            out[i, rows:, :] = jnp.where(line < tail // 2, turned, ends)

    for full in range(kv.shape[0] + 1):
        pl.when(last == full)(functools.partial(body, full))


def finish_kernel(lam, gate, outer, insig, taps, head_gain, attn_w, conv_w, parts, mixed, totals):
    count, _, columns = parts.shape
    rows = gate.shape[0]
    value_size = columns // 2

    tails = [parts[j, rows:, :].astype(jnp.float32) for j in range(count)]
    logs = [t[0:2] + t[2:4] + t[4:6] for t in tails]
    top = logs[0]
    for log in logs[1:]:
        top = jnp.maximum(top, log)
    shares = [jnp.exp2(log - top) for log in logs]
    total = shares[0]
    for share in shares[1:]:
        total = total + share
    totals[0] = (jnp.log2(total) + top) * LN2
    shares = [share / total for share in shares]
    pad = jnp.zeros((value_size - 2 * count, rows), jnp.float32)
    turned = jnp.transpose(jnp.concatenate([*shares, pad], axis=0))
    slot = lax.rem(lax.axis_index("sp"), count)
    ends = parts[lax.rem(slot + count - 1, count), rows:, :].astype(jnp.float32)
    ends = jnp.where(slot == 0, ends[:, value_size:], ends[:, :value_size])
    reach = taps.shape[0] - 1
    signal = insig[...].astype(jnp.float32)
    row = lax.broadcasted_iota(jnp.int32, signal.shape, 0)
    convolved = taps[reach : reach + 1, :] * signal
    for by in range(1, reach + 1):
        moved = pltpu.roll(signal, by, axis=0)
        for at in range(by):
            line = ends.shape[0] - by + at
            moved = jnp.where(row == at, ends[line : line + 1, :], moved)
        convolved = convolved + taps[reach - by : reach - by + 1, :] * moved
    conv = (outer[...].astype(jnp.float32) * convolved).astype(jnp.bfloat16)
    mapped = [jnp.zeros((rows, value_size), jnp.float32) for _ in range(2)]
    for j in range(count):
        for m in range(2):
            piece = parts[j, :rows, m * value_size : (m + 1) * value_size].astype(jnp.float32)
            mapped[m] = mapped[m] + turned[:, 2 * j + m : 2 * j + m + 1] * piece
    diff = mapped[0] - lam[0] * mapped[1]
    norm = lax.rsqrt(jnp.mean(diff * diff, axis=-1, keepdims=True) + 1e-05)
    opened = gate[...].astype(jnp.float32)
    head = diff * norm * head_gain[...] * (opened / (1.0 + jnp.exp(-opened)))
    mixed[...] = (
        jnp.dot(head.astype(jnp.bfloat16), attn_w[...], preferred_element_type=jnp.float32)
        + jnp.dot(conv, conv_w[...], preferred_element_type=jnp.float32)
    ).astype(jnp.bfloat16)


VMEM = pl.BlockSpec(memory_space=pltpu.VMEM)
SMEM = pl.BlockSpec(memory_space=pltpu.SMEM)


def close(array):
    return pltpu.with_memory_space_constraint(array, pltpu.VMEM)


def project(own, other, gain, weights, copies, tail):
    rows = own.shape[1]
    width = gain.shape[0]
    columns = weights[0].shape[1]
    return pl.pallas_call(
        project_kernel,
        out_shape=(
            pltpu.VMEM((rows, 2 * columns), jnp.bfloat16),
            pltpu.VMEM((rows - rows // copies + tail, 2 * columns), jnp.bfloat16),
            pltpu.VMEM((copies, rows, columns), jnp.bfloat16),
            jax.ShapeDtypeStruct((rows, width), jnp.bfloat16),
            jax.ShapeDtypeStruct((rows, columns), jnp.float32),
        ),
        in_specs=[VMEM] * 8,
        out_specs=(VMEM,) * 5,
        name="project",
    )(close(own), gain.reshape(1, width), *weights, close(other))


def gates(normed, scale, weights):
    shape = jax.ShapeDtypeStruct((normed.shape[0], weights[0].shape[1]), jnp.bfloat16)
    return pl.pallas_call(
        gates_kernel,
        out_shape=(shape,) * 3,
        in_specs=[VMEM] * 6,
        out_specs=(VMEM,) * 3,
        cost_estimate=pl.CostEstimate(flops=8 * normed.size * weights[0].shape[1], transcendentals=0, bytes_accessed=4 * normed.size),
        name="gates",
    )(normed, scale, *weights)


def attend(queries, own, ending, moved, kv, chunk, extra):
    count, rows, _ = queries.shape
    others, _, wide = kv.shape
    span = 2

    def tiled(length, width):
        return pl.BlockSpec((span, length, width), lambda i: (i, 0, 0))

    return pl.pallas_call(
        functools.partial(attend_kernel, chunk, span),
        grid=(count // span,),
        out_shape=jax.ShapeDtypeStruct((count, rows + extra, wide), jnp.bfloat16),
        in_specs=[VMEM] * 5,
        out_specs=tiled(rows + extra, wide),
        scratch_shapes=[pltpu.VMEM((2, others + 1, rows, rows), jnp.float32)],
        name="attend",
    )(close(queries), close(own), close(ending), close(moved), close(kv))


def finish(parts, lambdas, gate, outer, insig, taps, head_gain, attn_w, conv_w):
    rows = gate.shape[0]
    return pl.pallas_call(
        finish_kernel,
        out_shape=(
            pltpu.VMEM((rows, attn_w.shape[1]), jnp.bfloat16),
            jax.ShapeDtypeStruct((1, 2, rows), jnp.float32),
        ),
        in_specs=[SMEM] + [VMEM] * 8,
        out_specs=(VMEM, VMEM),
        name="finish",
    )(lambdas, gate, outer, insig, taps, head_gain.reshape(1, -1), attn_w, conv_w, close(parts))


def earlier_blocks(block, shifted, groups, chunk):
    devices = lax.axis_size("sp")
    count = devices // chunk
    rows, wide = block.shape
    step = rows // count
    share = rows - step
    moved = lax.ppermute(shifted, "sp", [(i, i + chunk) for i in range(devices - chunk)])
    start = share - lax.div(lax.axis_index("sp"), chunk) * step
    held = lax.dynamic_slice_in_dim(jnp.concatenate([moved[:share], block], axis=0), start, share, 0)
    gathered = lax.all_gather(held, "sp", axis_index_groups=groups, tiled=True)
    return gathered.reshape(count - 1, rows, wide), moved


def per_device(
    tokens,
    norm_gain,
    query_weight,
    key_weight,
    value_weight,
    gate_weight,
    outer_weight,
    inner_weight,
    signal_weight,
    conv_taps,
    lambdas,
    head_gain,
    attn_out_weight,
    conv_out_weight,
):
    chunk = 8
    tp = lax.axis_size("tp")
    sp = lax.axis_size("sp")
    near = [[g * chunk + i for i in range(chunk)] for g in range(sp // chunk)]
    far = [[g * chunk + i for g in range(sp // chunk)] for i in range(chunk)]
    same_core = [[2 * x + c for x in range(tp // 2)] for c in range(2)]

    own = lax.all_gather(tokens, "tp", axis_index_groups=same_core)
    other = lax.ppermute(own, "tp", [(i, i ^ 1) for i in range(tp)])
    tail = 16
    kv, shifted, query, normed, scale = project(
        own,
        other,
        norm_gain,
        (query_weight, key_weight, value_weight, inner_weight, signal_weight),
        chunk,
        tail,
    )
    queries = lax.all_to_all(query, "sp", 0, 0, axis_index_groups=near, tiled=True)
    earlier, moved = earlier_blocks(kv, shifted, far, chunk)
    parts = attend(queries, kv, shifted, moved, earlier, chunk, tail)
    normed, parts = lax.optimization_barrier((normed, parts))
    gate, outer, insig = gates(normed, scale, (gate_weight, outer_weight, inner_weight, signal_weight))
    parts = lax.all_to_all(parts, "sp", 0, 0, axis_index_groups=near, tiled=True)
    partial, log_totals = finish(
        parts, lambdas, gate, outer, insig, conv_taps, head_gain, attn_out_weight, conv_out_weight
    )
    tiles = lax.all_to_all(partial.reshape(tp, -1, partial.shape[1]), "tp", 0, 0, tiled=True)
    mixed = jnp.sum(tiles.astype(jnp.float32), axis=0).astype(jnp.bfloat16)
    return mixed, log_totals


def solution(mesh):
    placed = (
        P("sp", "tp"),
        P(),
        P(None, "tp"),
        P(None, "tp"),
        P(None, "tp"),
        P(None, "tp"),
        P(None, "tp"),
        P(None, "tp"),
        P(None, "tp"),
        P(None, "tp"),
        P("tp"),
        P("tp"),
        P("tp", None),
        P("tp", None),
    )

    return jax.shard_map(
        per_device,
        mesh=mesh,
        in_specs=placed,
        out_specs=(P(("sp", "tp"), None), P("tp", None, "sp")),
        check_vma=False,
    )
```

```python
import functools

import jax
import jax.numpy as jnp
from jax import lax
from jax.experimental import pallas as pl
from jax.experimental.pallas import tpu as pltpu
from jax.sharding import PartitionSpec as P


LOG2E = 1.4426950408889634
LN2 = 0.6931471805599453
HIDDEN = -1e30


def project_kernel(own, gain, qw, kw, vw, iw, sw, other, kv, shifted, q, normed, scaled):
    count, rows, part = own.shape
    width = normed.shape[1]
    skipped = rows // q.shape[0]
    tail = shifted.shape[0] + skipped - rows

    def spread(core):
        squares = jnp.zeros((rows, part), jnp.float32)
        for ref, side in ((own, core), (other, 1 - core)):
            for x in range(count):
                at = (2 * x + side) * part
                piece = ref[x].astype(jnp.float32)
                squares = squares + piece * piece
                normed[:, at : at + part] = (piece * gain[:, at : at + part]).astype(jnp.bfloat16)
        scale = lax.rsqrt(jnp.sum(squares, axis=-1, keepdims=True) / width + 1e-06)

        def project(weight, low=0, factor=None):
            raw = jnp.dot(normed[low:, :], weight[...], preferred_element_type=jnp.float32)
            raw = raw * scale[low:]
            if factor is not None:
                raw = raw * factor
            return raw.astype(jnp.bfloat16)

        columns = kw.shape[1]
        for n, weight in enumerate((kw, vw)):
            cut = slice(n * columns, (n + 1) * columns)
            values = project(weight)
            kv[:, cut] = values
            shifted[: rows - skipped, cut] = values[skipped:]
        low = rows - tail
        ending = project(iw, low).astype(jnp.float32) * project(sw, low).astype(jnp.float32)
        shifted[rows - skipped :, :columns] = ending.astype(jnp.bfloat16)
        shifted[rows - skipped :, columns:] = jnp.zeros((tail, columns), jnp.bfloat16)
        query = project(qw, 0, LOG2E * (columns // 2) ** -0.5)
        for i in range(q.shape[0]):
            q[i] = query
        scaled[...] = jnp.broadcast_to(scale, scaled.shape)

    for core in range(2):
        pl.when(lax.rem(lax.axis_index("tp"), 2) == core)(functools.partial(spread, core))


def gates_kernel(normed, scale, gw, ow, iw, sw, gate, outer, insig):
    def project(weight):
        raw = jnp.dot(normed[...], weight[...], preferred_element_type=jnp.float32)
        return (raw * scale[...]).astype(jnp.bfloat16)

    insig[...] = (project(iw).astype(jnp.float32) * project(sw).astype(jnp.float32)).astype(jnp.bfloat16)
    outer[...] = project(ow)
    gate[...] = project(gw)


def attend_kernel(chunk, span, q, own, ending, moved, kv, out, held):
    rows = q.shape[1]
    columns = kv.shape[2]
    value_size = columns // 2
    key_size = value_size // 2
    index = lax.axis_index("sp")
    last = lax.div(index, chunk)
    slot = lax.rem(index, chunk)
    first = pl.program_id(0) * span
    lane = lax.broadcasted_iota(jnp.int32, (rows, value_size), 1)
    units = [(i, m) for i in range(span) for m in range(2)]

    def body(full):
        order = [*range(full), None]
        ones = jnp.ones((rows, value_size), jnp.bfloat16)
        row = lax.broadcasted_iota(jnp.int32, (rows, rows), 0)
        col = lax.broadcasted_iota(jnp.int32, (rows, rows), 1)

        def part(b, cut):
            return own[:, cut] if b is None else kv[b, :, cut]

        def seen(i):
            return row + (first + i - slot) * rows >= col

        def score(u, b):
            i, m = units[u]
            cut = slice(m * key_size, (m + 1) * key_size)
            s = lax.dot_general(
                q[first + i, :, cut], part(b, cut), (((1,), (1,)), ((), ())), preferred_element_type=jnp.float32
            )
            if b is None:
                s = jnp.where(seen(i), s, HIDDEN)
            held[u % 2, full if b is None else b] = s
            top = s[:, :value_size]
            for at in range(value_size, rows, value_size):
                top = jnp.maximum(top, s[:, at : at + value_size])
            return top

        def peak(tops):
            top = tops[0]
            for t in tops[1:]:
                top = jnp.maximum(top, t)
            return jnp.max(top, axis=-1, keepdims=True)

        stats = []
        top = peak([score(0, b) for b in order])
        for u, (i, m) in enumerate(units):
            ahead = []
            summed = jnp.zeros((rows, 2 * value_size), jnp.float32)
            for b in order:
                if u + 1 < len(units):
                    ahead.append(score(u + 1, b))
                w = jnp.exp2(held[u % 2, full if b is None else b] - top)
                if b is None:
                    w = jnp.where(seen(i), w, 0.0)
                values = jnp.concatenate([part(b, slice(value_size, None)), ones], axis=1)
                summed = summed + jnp.dot(w.astype(jnp.bfloat16), values, preferred_element_type=jnp.float32)
            total = summed[:, value_size:]
            some = total > 0.0
            safe = jnp.where(some, total, 1.0)
            out[i, :rows, m * value_size : (m + 1) * value_size] = (summed[:, :value_size] / safe).astype(
                jnp.bfloat16
            )
            stats.append(jnp.where(some, jnp.log2(safe) + top, HIDDEN))
            if ahead:
                top = peak(ahead)
        for i in range(span):
            spread = jnp.zeros((rows, value_size), jnp.float32)
            for m in range(2):
                rest = stats[2 * i + m]
                for piece in range(3):
                    rounded = rest.astype(jnp.bfloat16).astype(jnp.float32)
                    spread = jnp.where(lane == 2 * piece + m, rounded, spread)
                    rest = rest - rounded
            tail = out.shape[1] - rows
            turned = jnp.transpose(spread)[:tail].astype(jnp.bfloat16)
            ends = [ref[ref.shape[0] - tail :, :value_size] for ref in (ending, moved)]
            ends = jnp.concatenate(ends, axis=1)
            line = lax.broadcasted_iota(jnp.int32, (tail, columns), 0)
            out[i, rows:, :] = jnp.where(line < tail // 2, turned, ends)

    for full in range(kv.shape[0] + 1):
        pl.when(last == full)(functools.partial(body, full))


def finish_kernel(group, lam, gate, outer, insig, taps, head_gain, attn_w, conv_w, parts, theirs, kept, totals):
    count, _, columns = parts.shape
    rows = gate.shape[0]
    value_size = columns // 2

    tails = [parts[j, rows:, :].astype(jnp.float32) for j in range(count)]
    logs = [t[0:2] + t[2:4] + t[4:6] for t in tails]
    top = logs[0]
    for log in logs[1:]:
        top = jnp.maximum(top, log)
    shares = [jnp.exp2(log - top) for log in logs]
    total = shares[0]
    for share in shares[1:]:
        total = total + share
    totals[0] = (jnp.log2(total) + top) * LN2
    shares = [share / total for share in shares]
    pad = jnp.zeros((value_size - 2 * count, rows), jnp.float32)
    turned = jnp.transpose(jnp.concatenate([*shares, pad], axis=0))
    slot = lax.rem(lax.axis_index("sp"), count)
    ends = parts[lax.rem(slot + count - 1, count), rows:, :].astype(jnp.float32)
    ends = jnp.where(slot == 0, ends[:, value_size:], ends[:, :value_size])
    reach = taps.shape[0] - 1
    signal = insig[...].astype(jnp.float32)
    row = lax.broadcasted_iota(jnp.int32, signal.shape, 0)
    convolved = taps[reach : reach + 1, :] * signal
    for by in range(1, reach + 1):
        moved = pltpu.roll(signal, by, axis=0)
        for at in range(by):
            line = ends.shape[0] - by + at
            moved = jnp.where(row == at, ends[line : line + 1, :], moved)
        convolved = convolved + taps[reach - by : reach - by + 1, :] * moved
    conv = (outer[...].astype(jnp.float32) * convolved).astype(jnp.bfloat16)
    mapped = [jnp.zeros((rows, value_size), jnp.float32) for _ in range(2)]
    for j in range(count):
        for m in range(2):
            piece = parts[j, :rows, m * value_size : (m + 1) * value_size].astype(jnp.float32)
            mapped[m] = mapped[m] + turned[:, 2 * j + m : 2 * j + m + 1] * piece
    diff = mapped[0] - lam[0] * mapped[1]
    norm = lax.rsqrt(jnp.mean(diff * diff, axis=-1, keepdims=True) + 1e-05)
    opened = gate[...].astype(jnp.float32)
    head = diff * norm * head_gain[...] * (opened / (1.0 + jnp.exp(-opened)))
    side = lax.rem(lax.axis_index("tp"), 2)
    share = theirs.shape[0] // group
    halves = [
        jnp.reshape(part, (group, 2, share, part.shape[1])) for part in (head.astype(jnp.bfloat16), conv)
    ]

    def chosen(half, core):
        return jnp.where(core == 0, half[:, 0], half[:, 1]).reshape(group * share, half.shape[3])

    theirs[...] = (
        jnp.dot(chosen(halves[0], 1 - side), attn_w[...], preferred_element_type=jnp.float32)
        + jnp.dot(chosen(halves[1], 1 - side), conv_w[...], preferred_element_type=jnp.float32)
    ).astype(jnp.bfloat16)
    kept[:, :value_size] = chosen(halves[0], side)
    kept[:, value_size:] = chosen(halves[1], side)


def join_kernel(kept, received, attn_w, conv_w, out):
    size = attn_w.shape[0]
    out[...] = (
        jnp.dot(kept[:, :size], attn_w[...], preferred_element_type=jnp.float32)
        + jnp.dot(kept[:, size:], conv_w[...], preferred_element_type=jnp.float32)
        + received[...].astype(jnp.float32)
    ).astype(jnp.bfloat16)


VMEM = pl.BlockSpec(memory_space=pltpu.VMEM)
SMEM = pl.BlockSpec(memory_space=pltpu.SMEM)


def close(array):
    return pltpu.with_memory_space_constraint(array, pltpu.VMEM)


def project(own, other, gain, weights, copies, tail):
    rows = own.shape[1]
    width = gain.shape[0]
    columns = weights[0].shape[1]
    return pl.pallas_call(
        project_kernel,
        out_shape=(
            pltpu.VMEM((rows, 2 * columns), jnp.bfloat16),
            pltpu.VMEM((rows - rows // copies + tail, 2 * columns), jnp.bfloat16),
            pltpu.VMEM((copies, rows, columns), jnp.bfloat16),
            jax.ShapeDtypeStruct((rows, width), jnp.bfloat16),
            jax.ShapeDtypeStruct((rows, columns), jnp.float32),
        ),
        in_specs=[VMEM] * 8,
        out_specs=(VMEM,) * 5,
        name="project",
    )(close(own), gain.reshape(1, width), *weights, close(other))


def gates(normed, scale, weights):
    shape = jax.ShapeDtypeStruct((normed.shape[0], weights[0].shape[1]), jnp.bfloat16)
    return pl.pallas_call(
        gates_kernel,
        out_shape=(shape,) * 3,
        in_specs=[VMEM] * 6,
        out_specs=(VMEM,) * 3,
        cost_estimate=pl.CostEstimate(flops=8 * normed.size * weights[0].shape[1], transcendentals=0, bytes_accessed=4 * normed.size),
        name="gates",
    )(normed, scale, *weights)


def attend(queries, own, ending, moved, kv, chunk, extra):
    count, rows, _ = queries.shape
    others, _, wide = kv.shape
    span = 2

    def tiled(length, width):
        return pl.BlockSpec((span, length, width), lambda i: (i, 0, 0))

    return pl.pallas_call(
        functools.partial(attend_kernel, chunk, span),
        grid=(count // span,),
        out_shape=jax.ShapeDtypeStruct((count, rows + extra, wide), jnp.bfloat16),
        in_specs=[VMEM] * 5,
        out_specs=tiled(rows + extra, wide),
        scratch_shapes=[pltpu.VMEM((2, others + 1, rows, rows), jnp.float32)],
        name="attend",
    )(close(queries), close(own), close(ending), close(moved), close(kv))


def finish(group, parts, lambdas, gate, outer, insig, taps, head_gain, attn_w, conv_w):
    rows, size = gate.shape
    return pl.pallas_call(
        functools.partial(finish_kernel, group),
        out_shape=(
            pltpu.VMEM((rows // 2, attn_w.shape[1]), jnp.bfloat16),
            pltpu.VMEM((rows // 2, 2 * size), jnp.bfloat16),
            jax.ShapeDtypeStruct((1, 2, rows), jnp.float32),
        ),
        in_specs=[SMEM] + [VMEM] * 8,
        out_specs=(VMEM, VMEM, VMEM),
        name="finish",
    )(lambdas, gate, outer, insig, taps, head_gain.reshape(1, -1), attn_w, conv_w, close(parts))


def join(kept, received, attn_w, conv_w):
    return pl.pallas_call(
        join_kernel,
        out_shape=pltpu.VMEM(received.shape, jnp.bfloat16),
        in_specs=[VMEM] * 4,
        out_specs=VMEM,
        name="join",
    )(close(kept), close(received), attn_w, conv_w)


def earlier_blocks(block, shifted, groups, chunk):
    devices = lax.axis_size("sp")
    count = devices // chunk
    rows, wide = block.shape
    step = rows // count
    share = rows - step
    moved = lax.ppermute(shifted, "sp", [(i, i + chunk) for i in range(devices - chunk)])
    start = share - lax.div(lax.axis_index("sp"), chunk) * step
    held = lax.dynamic_slice_in_dim(jnp.concatenate([moved[:share], block], axis=0), start, share, 0)
    gathered = lax.all_gather(held, "sp", axis_index_groups=groups, tiled=True)
    return gathered.reshape(count - 1, rows, wide), moved


def per_device(
    tokens,
    norm_gain,
    query_weight,
    key_weight,
    value_weight,
    gate_weight,
    outer_weight,
    inner_weight,
    signal_weight,
    conv_taps,
    lambdas,
    head_gain,
    attn_out_weight,
    conv_out_weight,
):
    chunk = 8
    tp = lax.axis_size("tp")
    sp = lax.axis_size("sp")
    near = [[g * chunk + i for i in range(chunk)] for g in range(sp // chunk)]
    far = [[g * chunk + i for g in range(sp // chunk)] for i in range(chunk)]
    same_core = [[2 * x + c for x in range(tp // 2)] for c in range(2)]

    own = lax.all_gather(tokens, "tp", axis_index_groups=same_core)
    other = lax.ppermute(own, "tp", [(i, i ^ 1) for i in range(tp)])
    tail = 16
    kv, shifted, query, normed, scale = project(
        own,
        other,
        norm_gain,
        (query_weight, key_weight, value_weight, inner_weight, signal_weight),
        chunk,
        tail,
    )
    queries = lax.all_to_all(query, "sp", 0, 0, axis_index_groups=near, tiled=True)
    earlier, moved = earlier_blocks(kv, shifted, far, chunk)
    parts = attend(queries, kv, shifted, moved, earlier, chunk, tail)
    normed, parts = lax.optimization_barrier((normed, parts))
    gate, outer, insig = gates(normed, scale, (gate_weight, outer_weight, inner_weight, signal_weight))
    parts = lax.all_to_all(parts, "sp", 0, 0, axis_index_groups=near, tiled=True)
    theirs, kept, log_totals = finish(
        tp // 2, parts, lambdas, gate, outer, insig, conv_taps, head_gain, attn_out_weight, conv_out_weight
    )
    received = lax.ppermute(theirs, "tp", [(i, i ^ 1) for i in range(tp)])
    partial = join(kept, received, attn_out_weight, conv_out_weight)
    tiles = lax.all_to_all(
        partial.reshape(tp // 2, -1, partial.shape[1]), "tp", 0, 0, axis_index_groups=same_core, tiled=True
    )
    mixed = jnp.sum(tiles.astype(jnp.float32), axis=0).astype(jnp.bfloat16)
    return mixed, log_totals


def solution(mesh):
    placed = (
        P("sp", "tp"),
        P(),
        P(None, "tp"),
        P(None, "tp"),
        P(None, "tp"),
        P(None, "tp"),
        P(None, "tp"),
        P(None, "tp"),
        P(None, "tp"),
        P(None, "tp"),
        P("tp"),
        P("tp"),
        P("tp", None),
        P("tp", None),
    )

    return jax.shard_map(
        per_device,
        mesh=mesh,
        in_specs=placed,
        out_specs=(P(("sp", "tp"), None), P("tp", None, "sp")),
        check_vma=False,
    )
```
